32 devices in a mesh: sp: 8 (over z, x), tp: 4 (over y, core).
Axes of the slice: x: 2, y: 2, z: 4, core: 2. Of those that a mesh axis runs over, the one named last changes fastest.
Arguments:
- latent: bfloat16 [4096, 2048], P(('sp', 'tp')), may hold values from -6 to 6
- context: bfloat16 [512, 2048], P('sp'), may hold values from -6 to 6
- conditioning: float32 [2048], P('sp'), may hold values from -6 to 6
- context_conditioning: float32 [2048], P('sp'), may hold values from -6 to 6
- shift_weight: bfloat16 [2048, 2048], P('sp', 'tp'), may hold values from -0.25 to 0.25
- scale_weight: bfloat16 [2048, 2048], P('sp', 'tp'), may hold values from -0.25 to 0.25
- gate_weight: bfloat16 [2048, 2048], P('sp', 'tp'), may hold values from -0.25 to 0.25
- norm_gain: float32 [2048], replicated, may hold values from 0.1 to 1.9
- query_weight: bfloat16 [2048, 2048], P(None, 'tp'), may hold values from -0.125 to 0.125
- key_weight: bfloat16 [2048, 1024], P(None, 'tp'), may hold values from -0.125 to 0.125
- value_weight: bfloat16 [2048, 1024], P(None, 'tp'), may hold values from -0.125 to 0.125
- query_gain: float32 [64], replicated, may hold values from 2 to 64, as said below
- key_gain: float32 [64], replicated, may hold values from 0.1 to 1.9
- context_lift: float32 [32], P('tp'), may hold values from 1.5 to 3
- output_weight: bfloat16 [2048, 2048], P('tp'), may hold values from -0.125 to 0.125
Outputs:
- mixed: bfloat16 [4096, 2048], P(('sp', 'tp'))
The draws below stay inside these ranges and needn't reach their ends.
Inputs may be any that keep to these rules, and one draw needn't show every extreme that they name: `query_gain`: one gain for each channel of a head.
All inputs are finite; a program needn't handle non-finite values.
Results may differ from the reference program's by a relative error of at most 0.018.
The reference program's roundings to bfloat16 on the way count: a program that leaves them out, or rounds other values in their place, can miss the bound.
Values may be sent and summed in bfloat16 or wider, within the bound.
A program may use at most 128 MiB of HBM per device.

```python
import math
import jax
import jax.numpy as jnp
from jax import lax

D = 2048
HEAD = 64
Q_HEADS = 32
KV_HEADS = 16
GRID = 64
CTX = 512
TOKENS = 4096


def draw_query_gain(key, part):
    base_key = jax.random.fold_in(key, 0)
    gains = jax.random.uniform(base_key, (HEAD,), jnp.float32, 2.0, 3.5)
    return gains


def block_scale(own_key, shape, cuts, smallest, largest):
    level = 1.0
    for dim, shards_of in cuts:
        steps = jax.random.uniform(jax.random.fold_in(jax.random.fold_in(own_key, 6), dim), (shards_of,), jnp.float32, smallest / len(cuts), largest / len(cuts))
        level = level * jnp.repeat(jnp.exp(steps), shape[dim] // shards_of).reshape((-1,) + (1,) * (len(shape) - 1 - dim))
    return level


def gaussian(key, shape, spread, reach, cuts=(), held_as=jnp.bfloat16):
    values = jax.random.normal(key, shape, jnp.float32) * spread
    if len(cuts) > 0:
        values = block_scale(key, shape, cuts, -0.22, 0.18) * values
    return jnp.clip(values, min=-reach, max=reach).astype(held_as)


def setup_inputs(seed: int = 0) -> dict:
    arg_keys = jax.random.split(jax.random.key(seed), 16)
    return {
        "latent": gaussian(arg_keys[0], (TOKENS, D), 1.0, 6.0, ((0, 32),)),
        "context": gaussian(arg_keys[1], (CTX, D), 1.0, 6.0, ((0, 8),)),
        "conditioning": gaussian(arg_keys[2], (D,), 1.0, 6.0, ((0, 8),), jnp.float32),
        "context_conditioning": gaussian(arg_keys[3], (D,), 1.0, 6.0, ((0, 8),), jnp.float32),
        "shift_weight": gaussian(arg_keys[4], (D, D), (D // 4) ** -0.5, 0.25, ((0, 8), (1, 4))),
        "scale_weight": gaussian(arg_keys[5], (D, D), (D // 4) ** -0.5, 0.25, ((0, 8), (1, 4))),
        "gate_weight": gaussian(arg_keys[6], (D, D), (D // 4) ** -0.5, 0.25, ((0, 8), (1, 4))),
        "norm_gain": jnp.clip(1.0 + 0.18 * jax.random.normal(arg_keys[7], (D,), jnp.float32), 0.1, 1.9),
        "query_weight": gaussian(arg_keys[8], (D, Q_HEADS * HEAD), D ** -0.5, 0.125, ((1, 4),)),
        "key_weight": gaussian(arg_keys[9], (D, KV_HEADS * HEAD), D ** -0.5, 0.125, ((1, 4),)),
        "value_weight": gaussian(arg_keys[10], (D, KV_HEADS * HEAD), D ** -0.5, 0.125, ((1, 4),)),
        "query_gain": draw_query_gain(jax.random.fold_in(arg_keys[15], 71), 0),
        "key_gain": jnp.clip(1.0 + 0.18 * jax.random.normal(arg_keys[12], (HEAD,), jnp.float32), 0.1, 1.9),
        "context_lift": jnp.clip(1.5 + 1.5 * jax.random.uniform(arg_keys[13], (Q_HEADS,), jnp.float32) ** block_scale(arg_keys[13], (Q_HEADS,), ((0, 4),), -0.2, 0.2), 1.5, 3.0),
        "output_weight": gaussian(arg_keys[14], (Q_HEADS * HEAD, D), (Q_HEADS * HEAD) ** -0.5, 0.125, ((0, 4),)),
    }


EPSILON = 1e-06
ROTARY_BASE = 10000.0

def normalize(values, gain):
    return values * lax.rsqrt(lax.optimization_barrier(jnp.mean(values * values, axis=-1, keepdims=True)) + EPSILON) * gain

def rotary_tables(offset, count):
    position = offset + jnp.arange(count, dtype=jnp.int32)
    grid_row = (position // GRID).astype(jnp.float32)
    grid_column = (position % GRID).astype(jnp.float32)
    quarter = HEAD // 4
    frequency = ROTARY_BASE ** (-jnp.arange(quarter, dtype=jnp.float32) / quarter)
    angles = jnp.concatenate([grid_row[:, None] * frequency, grid_column[:, None] * frequency], axis=1)
    return (jnp.repeat(jnp.cos(angles), 2, axis=1), jnp.repeat(jnp.sin(angles), 2, axis=1))

def rotate(values, cos_table, sin_table):
    pairs = values.reshape(values.shape[:-1] + (HEAD // 2, 2))
    turned = jnp.stack([-pairs[..., 1], pairs[..., 0]], axis=-1).reshape(values.shape)
    return values * cos_table[:, None, :] + turned * sin_table[:, None, :]

def attend_head(operands):
    head_queries, head_keys, head_values, head_context_keys, head_context_values, lift = operands
    tokens = head_queries.shape[0]
    group = head_queries.shape[1]
    block = math.gcd(tokens, 512)
    keys_wide = head_keys.astype(jnp.float32)
    values_wide = head_values.astype(jnp.float32)
    context_keys_wide = head_context_keys.astype(jnp.float32)
    context_values_wide = head_context_values.astype(jnp.float32)

    def one_block(query_block):
        query_wide = query_block.astype(jnp.float32)
        latent_scores = jnp.einsum('qgd,sd->gqs', query_wide, keys_wide) * HEAD ** (-0.5)
        context_scores = jnp.einsum('qgd,sd->gqs', query_wide, context_keys_wide) * HEAD ** (-0.5) + lift[:, None, None]
        top = jnp.maximum(lax.optimization_barrier(jnp.max(latent_scores, axis=-1)), lax.optimization_barrier(jnp.max(context_scores, axis=-1)))[..., None]
        latent_weights = jnp.exp(latent_scores - top)
        context_weights = jnp.exp(context_scores - top)
        total = lax.optimization_barrier(jnp.sum(latent_weights, axis=-1)) + lax.optimization_barrier(jnp.sum(context_weights, axis=-1))
        summed = jnp.einsum('gqs,sd->qgd', latent_weights.astype(jnp.bfloat16).astype(jnp.float32), values_wide)
        summed = summed + jnp.einsum('gqs,sd->qgd', context_weights.astype(jnp.bfloat16).astype(jnp.float32), context_values_wide)
        return (summed / jnp.transpose(total)[:, :, None]).astype(jnp.bfloat16)
    result = lax.map(one_block, head_queries.reshape(tokens // block, block, group, HEAD))
    return result.reshape(tokens, group, HEAD)

def reference(latent, context, conditioning, context_conditioning, shift_weight, scale_weight, gate_weight, norm_gain, query_weight, key_weight, value_weight, query_gain, key_gain, context_lift, output_weight):
    signals = jnp.stack([jax.nn.silu(conditioning), jax.nn.silu(context_conditioning)]).astype(jnp.bfloat16)
    shifts = jnp.dot(signals, shift_weight, preferred_element_type=jnp.float32)
    scales = jnp.dot(signals, scale_weight, preferred_element_type=jnp.float32)
    gate = jnp.dot(signals[0:1], gate_weight, preferred_element_type=jnp.float32)[0]
    hidden = (normalize(latent.astype(jnp.float32), norm_gain) * (1.0 + scales[0]) + shifts[0]).astype(jnp.bfloat16)
    context_hidden = (normalize(context.astype(jnp.float32), norm_gain) * (1.0 + scales[1]) + shifts[1]).astype(jnp.bfloat16)
    tokens = latent.shape[0]
    group = Q_HEADS // KV_HEADS
    cos_table, sin_table = rotary_tables(0, tokens)
    raw_queries = jnp.dot(hidden, query_weight, preferred_element_type=jnp.float32).reshape(tokens, Q_HEADS, HEAD)
    queries = rotate(normalize(raw_queries, query_gain), cos_table, sin_table).astype(jnp.bfloat16)
    raw_keys = jnp.dot(hidden, key_weight, preferred_element_type=jnp.float32).reshape(tokens, KV_HEADS, HEAD)
    keys = rotate(normalize(raw_keys, key_gain), cos_table, sin_table).astype(jnp.bfloat16)
    values = jnp.dot(hidden, value_weight, preferred_element_type=jnp.float32).astype(jnp.bfloat16).reshape(tokens, KV_HEADS, HEAD)
    raw_context_keys = jnp.dot(context_hidden, key_weight, preferred_element_type=jnp.float32).reshape(CTX, KV_HEADS, HEAD)
    context_keys = normalize(raw_context_keys, key_gain).astype(jnp.bfloat16)
    context_values = jnp.dot(context_hidden, value_weight, preferred_element_type=jnp.float32).astype(jnp.bfloat16).reshape(CTX, KV_HEADS, HEAD)
    operands = (jnp.transpose(queries.reshape(tokens, KV_HEADS, group, HEAD), (1, 0, 2, 3)), jnp.transpose(keys, (1, 0, 2)), jnp.transpose(values, (1, 0, 2)), jnp.transpose(context_keys, (1, 0, 2)), jnp.transpose(context_values, (1, 0, 2)), context_lift.reshape(KV_HEADS, group))
    attended = lax.map(attend_head, operands)
    attended = jnp.transpose(attended, (1, 0, 2, 3)).reshape(tokens, Q_HEADS * HEAD)
    projection = jnp.dot(attended, output_weight, preferred_element_type=jnp.float32)
    return (latent.astype(jnp.float32) + gate * projection).astype(jnp.bfloat16)
```

```python
import functools

import jax
import jax.numpy as jnp
from jax import lax
from jax.experimental import pallas as pl
from jax.experimental.pallas import tpu as pltpu
from jax.sharding import PartitionSpec as P

HEAD = 64
GRID = 64
EPSILON = 1e-06
ROTARY_BASE = 10000.0
F32 = jnp.float32
BF16 = jnp.bfloat16
VMEM = pltpu.VMEM


def dot(a, b):
    return jnp.dot(a, b, preferred_element_type=F32)


def remote(src, dst, send, recv, sp, tp):
    return pltpu.make_async_remote_copy(
        src_ref=src,
        dst_ref=dst,
        send_sem=send,
        recv_sem=recv,
        device_id=(sp, tp),
        device_id_type=pl.DeviceIdType.MESH,
    )


def project_kernel(
    n_sp, n_tp, q_heads, k_heads,
    latent, context, cond, ctx_cond, shift_w, scale_w, gate_w, gain,
    wq, wk, wv, q_gain, k_gain, cos_t, sin_t,
    qz, kv, ckv, gate_out,
    lat, part, total, recv1, recv2, mods,
    s1, r1, s2, r2, sy, ry, sp_own, sp_fwd, rp,
):
    me = lax.axis_index("sp")
    t = lax.axis_index("tp")
    n_y = n_tp // 2
    y, c = t // 2, t % 2
    partner = y * 2 + 1 - c
    barrier = pltpu.get_barrier_semaphore()

    def greet_sp(j, _):
        pl.semaphore_signal(barrier, inc=1, device_id=(lax.rem(me + j, n_sp), t), device_id_type=pl.DeviceIdType.MESH)
        return 0

    def greet_tp(j, _):
        pl.semaphore_signal(barrier, inc=1, device_id=(me, lax.rem(t + j, n_tp)), device_id_type=pl.DeviceIdType.MESH)
        return 0

    lax.fori_loop(1, n_sp, greet_sp, 0)
    lax.fori_loop(1, n_tp, greet_tp, 0)
    pl.semaphore_wait(barrier, n_sp + n_tp - 2)

    def y_copy(k):
        other = lax.rem(y + k, n_y)
        return remote(latent, lat.at[t], sy.at[k], ry.at[t], me, other * 2 + c)

    def y_start(k, _):
        y_copy(k).start()
        return 0

    lax.fori_loop(1, n_y, y_start, 0)
    own_partner = remote(latent, lat.at[t], sp_own, rp.at[t], me, partner)
    own_partner.start()

    rows = lax.broadcasted_iota(jnp.int32, (8, cond.shape[1]), 0)
    a = jnp.broadcast_to(cond[...] / (1.0 + jnp.exp(-cond[...])), rows.shape)
    b = jnp.broadcast_to(ctx_cond[...] / (1.0 + jnp.exp(-ctx_cond[...])), rows.shape)
    first = jnp.where(rows == 0, a, jnp.where(rows == 1, b, 0.0)).astype(BF16)
    second = jnp.where(rows == 2, a, jnp.where(rows == 3, b, 0.0)).astype(BF16)
    third = jnp.where(rows == 4, a, 0.0).astype(BF16)
    mine = dot(first, shift_w[...]) + dot(second, scale_w[...]) + dot(third, gate_w[...])
    part[...] = mine
    recv1[me] = mine

    def mod_copy(j):
        return remote(part, recv1.at[me], s1.at[j], r1.at[me], lax.rem(me + j, n_sp), t)

    def mod_start(j, _):
        mod_copy(j).start()
        return 0

    def mod_wait(j, _):
        src = lax.rem(me + j, n_sp)
        pltpu.make_async_copy(recv1.at[src], recv1.at[src], r1.at[src]).wait()
        return 0

    lax.fori_loop(1, n_sp, mod_start, 0)
    lax.fori_loop(1, n_sp, mod_wait, 0)
    summed = lax.fori_loop(1, n_sp, lambda j, s: s + recv1[j], recv1[0])
    total[...] = summed
    recv2[t] = summed

    def tot_copy(j):
        return remote(total, recv2.at[t], s2.at[j], r2.at[t], me, lax.rem(t + j, n_tp))

    def tot_start(j, _):
        tot_copy(j).start()
        return 0

    def tot_wait(j, _):
        src = lax.rem(t + j, n_tp)
        pltpu.make_async_copy(recv2.at[src], recv2.at[src], r2.at[src]).wait()
        return 0

    lax.fori_loop(1, n_tp, tot_start, 0)
    lax.fori_loop(1, n_tp, tot_wait, 0)
    width = total.shape[1]
    for j in range(n_tp):
        mods[:, j * width : (j + 1) * width] = recv2[j]
    gate_out[...] = mods[4:5, :]

    def hidden_of(x, shift_row, scale_row):
        x = x.astype(F32)
        inv = lax.rsqrt(jnp.mean(x * x, axis=-1, keepdims=True) + EPSILON)
        return (
            x * inv * gain[...] * (1.0 + mods[scale_row : scale_row + 1, :])
            + mods[shift_row : shift_row + 1, :]
        ).astype(BF16)

    def head_norm(v, gains):
        w = v.shape[1]
        heads_r = lax.broadcasted_iota(jnp.int32, (w, w), 0) // HEAD
        heads_c = lax.broadcasted_iota(jnp.int32, (w, w), 1) // HEAD
        ones = jnp.where(heads_r == heads_c, 1.0, 0.0).astype(BF16)
        sq = v * v
        hi = sq.astype(BF16)
        rest = sq - hi.astype(F32)
        mid = rest.astype(BF16)
        low = (rest - mid.astype(F32)).astype(BF16)
        mean = (dot(hi, ones) + (dot(mid, ones) + dot(low, ones))) * (1.0 / HEAD)
        return v * lax.rsqrt(mean + EPSILON) * jnp.concatenate([gains] * (w // 128), axis=1)

    def turn(v, cos_v, sin_v):
        w = v.shape[1]
        even = lax.broadcasted_iota(jnp.int32, v.shape, 1) % 2 == 0
        swapped = jnp.where(even, pltpu.roll(v, w - 1, 1), pltpu.roll(v, 1, 1))
        many = w // 128
        return v * jnp.concatenate([cos_v] * many, axis=1) + swapped * jnp.concatenate([sin_v] * many, axis=1)

    k_width = wk.shape[1]
    group = q_heads // k_heads

    def process(tile, x):
        h = hidden_of(x, 0, 2)
        cos_v, sin_v = cos_t[tile], sin_t[tile]
        q = turn(head_norm(dot(h, wq[...]), q_gain[...]), cos_v, sin_v)
        low_half = lax.broadcasted_iota(jnp.int32, (q.shape[0], 128), 1) < HEAD
        for head in range(q_heads):
            piece = q[:, (head // 2) * 128 : (head // 2) * 128 + 128].astype(BF16).astype(F32) * HEAD ** (-0.5)
            side = (head // group) % 2
            if head % 2 != side:
                piece = pltpu.roll(piece, HEAD, 1)
            keep = low_half if side == 0 else jnp.logical_not(low_half)
            qz[head, tile] = jnp.where(keep, piece, 0.0).astype(BF16)
        k = turn(head_norm(dot(h, wk[...]), k_gain[...]), cos_v, sin_v)
        kv[tile, :, :k_width] = k.astype(BF16)
        kv[tile, :, k_width:] = dot(h, wv[...]).astype(BF16)

    hc = hidden_of(context[...], 1, 3)
    ckv[:, :k_width] = head_norm(dot(hc, wk[...]), k_gain[...]).astype(BF16)
    ckv[:, k_width:] = dot(hc, wv[...]).astype(BF16)

    process(t, latent[...])
    pltpu.make_async_copy(lat.at[partner], lat.at[partner], rp.at[partner]).wait()
    process(partner, lat[partner])

    def others(k, _):
        other = lax.rem(y + n_y - k, n_y)
        near, far = other * 2 + c, other * 2 + 1 - c
        pltpu.make_async_copy(lat.at[near], lat.at[near], ry.at[near]).wait()
        remote(lat.at[near], lat.at[near], sp_fwd.at[k], rp.at[near], me, partner).start()
        process(near, lat[near])
        pltpu.make_async_copy(lat.at[far], lat.at[far], rp.at[far]).wait()
        process(far, lat[far])
        return 0

    lax.fori_loop(1, n_y, others, 0)

    def drain_y(k, _):
        y_copy(k).wait_send()
        other = lax.rem(y + n_y - k, n_y)
        near = other * 2 + c
        remote(lat.at[near], lat.at[near], sp_fwd.at[k], rp.at[near], me, partner).wait_send()
        return 0

    lax.fori_loop(1, n_y, drain_y, 0)
    own_partner.wait_send()

    def drain_1(j, _):
        mod_copy(j).wait_send()
        return 0

    def drain_2(j, _):
        tot_copy(j).wait_send()
        return 0

    lax.fori_loop(1, n_sp, drain_1, 0)
    lax.fori_loop(1, n_tp, drain_2, 0)


def ring_position(index, n_z, n_x):
    z, x = index // n_x, index % n_x
    back = n_z * (n_x - 1) + n_z - 1 - z
    out = z * (n_x - 1) + jnp.where(z % 2 == 0, x - 1, n_x - 1 - x)
    return jnp.where(x == 0, back, out)


def ring_index(place, n_z, n_x):
    r, k = place // (n_x - 1), place % (n_x - 1)
    out = r * n_x + jnp.where(r % 2 == 0, 1 + k, n_x - 1 - k)
    back = (n_z - 1 - (place - n_z * (n_x - 1))) * n_x
    return jnp.where(place >= n_z * (n_x - 1), back, out)


def attend_kernel(
    n_sp, n_tp, n_x, q_heads, k_heads, chunks,
    qz, kv, ckv, lift, wo,
    by_rows, wo_all,
    right, left, cbuf, m_ref, acc, att,
    s_kv, r_kv, s_c, r_c, s_wy, r_wy, s_wp, r_wp, s_a, r_a, loc,
):
    me = lax.axis_index("sp")
    t = lax.axis_index("tp")
    n_y = n_tp // 2
    y, c = t // 2, t % 2
    partner = y * 2 + 1 - c
    half = n_sp // 2
    if n_x > 1:
        n_z = n_sp // n_x
        place = ring_position(me, n_z, n_x)
        nxt = ring_index(lax.rem(place + 1, n_sp), n_z, n_x)
        prv = ring_index(lax.rem(place + n_sp - 1, n_sp), n_z, n_x)
    else:
        nxt, prv = lax.rem(me + 1, n_sp), lax.rem(me + n_sp - 1, n_sp)
    barrier = pltpu.get_barrier_semaphore()
    for peer in (nxt, prv):
        pl.semaphore_signal(barrier, inc=1, device_id=(peer, t), device_id_type=pl.DeviceIdType.MESH)

    def greet(j, _):
        pl.semaphore_signal(barrier, inc=1, device_id=(me, lax.rem(t + j, n_tp)), device_id_type=pl.DeviceIdType.MESH)
        return 0

    lax.fori_loop(1, n_tp, greet, 0)
    pl.semaphore_wait(barrier, 2 + n_tp - 1)

    length = kv.shape[0]
    mid = length // 2

    def hop(src, dst, direction, i):
        return remote(src, dst, s_kv.at[direction, i], r_kv.at[direction, i], nxt if direction == 0 else prv, t)

    def chop(src, dst, direction, i):
        return remote(src, dst, s_c.at[direction, i], r_c.at[direction, i], nxt if direction == 0 else prv, t)

    def sends(i, source_r, source_l, c_r, c_l):
        return (
            hop(source_r, right.at[i], 0, i),
            hop(source_l, left.at[i], 1, i),
            chop(c_r, cbuf.at[i], 0, i),
            chop(c_l, cbuf.at[n_sp - i], 1, i),
        )

    def last_sends(source_r, source_l, c_r):
        return (
            hop(source_r.at[pl.ds(0, mid)], right.at[half, pl.ds(0, mid)], 0, half),
            hop(source_l.at[pl.ds(mid, mid)], right.at[half, pl.ds(mid, mid)], 1, half),
            chop(c_r, cbuf.at[half], 0, half),
        )

    opening = sends(1, kv, kv, ckv, ckv)
    for copy in opening:
        copy.start()
    own_c = pltpu.make_async_copy(ckv, cbuf.at[0], loc.at[0])
    own_c.start()
    own_w = pltpu.make_async_copy(wo, wo_all.at[t], loc.at[1])
    own_w.start()

    def w_y(k, ch):
        other = lax.rem(y + k, n_y)
        return remote(wo.at[ch], wo_all.at[t, ch], s_wy.at[k, ch], r_wy.at[t, ch], me, other * 2 + c)

    def w_own(ch):
        return remote(wo.at[ch], wo_all.at[t, ch], s_wp.at[0, ch], r_wp.at[t, ch], me, partner)

    def w_fwd(k, ch):
        other = lax.rem(y + n_y - k, n_y)
        near = other * 2 + c
        return remote(wo_all.at[near, ch], wo_all.at[near, ch], s_wp.at[k, ch], r_wp.at[near, ch], me, partner)

    for ch in range(chunks):
        for k in range(1, n_y):
            w_y(k, ch).start()
    for ch in range(chunks):
        w_own(ch).start()

    def forward_weight(ch):
        for k in range(1, n_y):
            other = lax.rem(y + n_y - k, n_y)
            near = other * 2 + c
            pltpu.make_async_copy(wo_all.at[near, ch], wo_all.at[near, ch], r_wy.at[near, ch]).wait()
            w_fwd(k, ch).start()

    k_width = kv.shape[1] // 2
    group = q_heads // k_heads
    tile = min(256, length)
    tiles = length // tile

    def attend(blocks, start, lifted):
        def one(step, _):
            head = step // tiles
            row = pl.multiple_of(lax.rem(step, tiles) * tile, tile)
            pair = head // (2 * group)
            lane = pl.multiple_of(pair * 128, 128)
            q = qz[head, pl.ds(row, tile), :]
            extra = lift[head]
            scores = []
            for pos, block in enumerate(blocks):
                s = lax.dot_general(
                    q, block[:, pl.ds(lane, 128)], (((1,), (1,)), ((), ())), preferred_element_type=F32
                )
                scores.append(s)
            tops = [jnp.max(s, axis=-1, keepdims=True) for s in scores]
            if lifted:
                tops[-1] = tops[-1] + extra
            top = functools.reduce(jnp.maximum, tops)
            if not start:
                old = m_ref[head, pl.ds(row, tile), :]
                top = jnp.maximum(old[:, 0:1], top)
            out = None
            for pos, block in enumerate(blocks):
                base = top - extra if lifted and pos == len(blocks) - 1 else top
                p = jnp.exp(scores[pos] - base).astype(BF16)
                v = block[:, pl.ds(pl.multiple_of(k_width + lane, 128), 128)]
                term = dot(p, jnp.concatenate([v, jnp.ones_like(v)], axis=1))
                out = term if out is None else out + term
            if not start:
                wide = jnp.broadcast_to(top, old.shape)
                f = jnp.exp(old - wide)
                out = acc[head, pl.ds(row, tile), :] * jnp.concatenate([f, f], axis=1) + out
                m_ref[head, pl.ds(row, tile), :] = wide
            else:
                m_ref[head, pl.ds(row, tile), :] = jnp.broadcast_to(top, (tile, 128))
            acc[head, pl.ds(row, tile), :] = out
            return 0

        lax.fori_loop(0, q_heads * tiles, one, 0)

    attend([kv], True, False)

    def wait_pair(i):
        for copy in sends(i, kv, kv, ckv, ckv):
            copy.wait_recv()

    def step(i, _):
        wait_pair(i)
        for copy in sends(i + 1, right.at[i], left.at[i], cbuf.at[i], cbuf.at[n_sp - i]):
            copy.start()
        attend([right.at[i], left.at[i]], False, False)
        forward_weight(i - 1)
        return 0

    lax.fori_loop(1, half - 1, step, 0)
    wait_pair(half - 1)
    closing = last_sends(right.at[half - 1], left.at[half - 1], cbuf.at[half - 1])
    for copy in closing:
        copy.start()
    attend([right.at[half - 1], left.at[half - 1]], False, False)
    for ch in range(half - 2, chunks):
        forward_weight(ch)
    for copy in closing:
        copy.wait_recv()
    own_c.wait()
    cflat = cbuf.reshape(n_sp * ckv.shape[0], ckv.shape[1])
    attend([right.at[half], cflat], False, True)

    low_half = lax.broadcasted_iota(jnp.int32, (length, 128), 1) < HEAD
    per = length // n_tp

    def normal(head):
        return acc[head, :, :128] / acc[head, :, 128:]

    for two in range(q_heads // 2):
        parts = []
        for head in (2 * two, 2 * two + 1):
            o = normal(head)
            if (head // group) % 2 != head % 2:
                o = pltpu.roll(o, HEAD, 1)
            parts.append(o)
        both = jnp.where(low_half, parts[0], parts[1]).astype(BF16)
        for j in range(n_tp):
            att[j, :, two * 128 : two * 128 + 128] = both[j * per : (j + 1) * per, :]

    def a_copy(j):
        to = lax.rem(t + j, n_tp)
        return remote(att.at[to], by_rows.at[t], s_a.at[j], r_a.at[t], me, to)

    for j in range(1, n_tp):
        a_copy(j).start()
    own_a = pltpu.make_async_copy(att.at[t], by_rows.at[t], loc.at[2])
    own_a.start()
    own_a.wait()
    for j in range(1, n_tp):
        src = lax.rem(t + j, n_tp)
        pltpu.make_async_copy(by_rows.at[src], by_rows.at[src], r_a.at[src]).wait()
    own_w.wait()
    for ch in range(chunks):
        for k in range(n_y):
            far = lax.rem(y + n_y - k, n_y) * 2 + 1 - c
            pltpu.make_async_copy(wo_all.at[far, ch], wo_all.at[far, ch], r_wp.at[far, ch]).wait()
        for k in range(1, n_y):
            w_y(k, ch).wait_send()
            w_fwd(k, ch).wait_send()
        w_own(ch).wait_send()
    for j in range(1, n_tp):
        a_copy(j).wait_send()

    def drain(i, _):
        for copy in sends(i, kv, kv, ckv, ckv):
            copy.wait_send()
        return 0

    lax.fori_loop(1, half, drain, 0)
    for copy in closing:
        copy.wait_send()


def rotary_tables(offset, count):
    position = offset + jnp.arange(count, dtype=jnp.int32)
    grid_row = (position // GRID).astype(F32)
    grid_column = (position % GRID).astype(F32)
    quarter = HEAD // 4
    frequency = ROTARY_BASE ** (-jnp.arange(quarter, dtype=F32) / quarter)
    angles = jnp.concatenate([grid_row[:, None] * frequency, grid_column[:, None] * frequency], axis=1)
    sign = jnp.where(jnp.arange(HEAD) % 2 == 0, -1.0, 1.0)
    cos_t, sin_t = jnp.repeat(jnp.cos(angles), 2, axis=1), jnp.repeat(jnp.sin(angles), 2, axis=1) * sign
    return jnp.tile(cos_t, (1, 2)), jnp.tile(sin_t, (1, 2))


def shards(
    n_sp, n_tp, n_x,
    latent, context, conditioning, context_conditioning, shift_weight, scale_weight, gate_weight,
    norm_gain, query_weight, key_weight, value_weight, query_gain, key_gain, context_lift, output_weight,
):
    k_heads = key_weight.shape[1] // HEAD
    q_heads = query_weight.shape[1] // HEAD
    if k_heads % 2:
        key_weight = jnp.pad(key_weight, ((0, 0), (0, HEAD)))
        value_weight = jnp.pad(value_weight, ((0, 0), (0, HEAD)))
    rows, model = latent.shape
    length = rows * n_tp
    k_width = key_weight.shape[1]
    c_rows = context.shape[0]
    part_width = shift_weight.shape[1]
    cos_t, sin_t = rotary_tables(lax.axis_index("sp") * length, length)
    vmem = pl.BlockSpec(memory_space=VMEM)
    dma = pltpu.SemaphoreType.DMA
    qz, kv, ckv, gate = pl.pallas_call(
        functools.partial(project_kernel, n_sp, n_tp, q_heads, k_heads),
        name="project",
        out_shape=(
            jax.ShapeDtypeStruct((q_heads, n_tp, rows, 128), BF16),
            jax.ShapeDtypeStruct((n_tp, rows, 2 * k_width), BF16),
            jax.ShapeDtypeStruct((c_rows, 2 * k_width), BF16),
            jax.ShapeDtypeStruct((1, model), F32),
        ),
        in_specs=[vmem] * 15,
        out_specs=(vmem,) * 4,
        scratch_shapes=[
            VMEM((n_tp, rows, model), BF16),
            VMEM((8, part_width), F32),
            VMEM((8, part_width), F32),
            VMEM((n_sp, 8, part_width), F32),
            VMEM((n_tp, 8, part_width), F32),
            VMEM((8, model), F32),
            dma((n_sp,)), dma((n_sp,)), dma((n_tp,)), dma((n_tp,)),
            dma((n_tp,)), dma((n_tp,)), dma, dma((n_tp,)), dma((n_tp,)),
        ],
        compiler_params=pltpu.CompilerParams(
            collective_id=0, has_side_effects=True, vmem_limit_bytes=48 * 1024 * 1024
        ),
    )(
        latent, context, conditioning[None], context_conditioning[None],
        shift_weight, scale_weight, gate_weight, norm_gain[None],
        query_weight, key_weight, value_weight,
        jnp.tile(query_gain, 2)[None], jnp.tile(key_gain, 2)[None],
        cos_t.reshape(n_tp, rows, 128), sin_t.reshape(n_tp, rows, 128),
    )
    chunks = max(n_sp // 2, 2)
    o_rows = output_weight.shape[0]
    by_rows, wo_all = pl.pallas_call(
        functools.partial(attend_kernel, n_sp, n_tp, n_x, q_heads, k_heads, chunks),
        name="attend",
        out_shape=(
            jax.ShapeDtypeStruct((n_tp, rows, q_heads * HEAD), BF16),
            jax.ShapeDtypeStruct((n_tp, chunks, o_rows // chunks, model), BF16),
        ),
        in_specs=[vmem, vmem, vmem, pl.BlockSpec(memory_space=pltpu.SMEM), vmem],
        out_specs=(vmem, pl.BlockSpec(memory_space=pl.ANY)),
        scratch_shapes=[
            VMEM((n_sp // 2 + 1, length, 2 * k_width), BF16),
            VMEM((n_sp // 2, length, 2 * k_width), BF16),
            VMEM((n_sp, c_rows, 2 * k_width), BF16),
            VMEM((q_heads, length, 128), F32),
            VMEM((q_heads, length, 256), F32),
            VMEM((n_tp, rows, q_heads * HEAD), BF16),
            dma((2, n_sp)), dma((2, n_sp)), dma((2, n_sp)), dma((2, n_sp)),
            dma((n_tp, chunks)), dma((n_tp, chunks)), dma((n_tp, chunks)), dma((n_tp, chunks)),
            dma((n_tp,)), dma((n_tp,)), dma((3,)),
        ],
        compiler_params=pltpu.CompilerParams(
            collective_id=1, has_side_effects=True, vmem_limit_bytes=56 * 1024 * 1024
        ),
    )(
        qz.reshape(q_heads, length, 128), kv.reshape(length, 2 * k_width), ckv, context_lift,
        output_weight.reshape(chunks, o_rows // chunks, model),
    )
    projection = jnp.dot(
        jnp.transpose(by_rows, (1, 0, 2)).reshape(rows, n_tp * o_rows),
        wo_all.reshape(n_tp * o_rows, model),
        preferred_element_type=F32,
    )
    return (latent.astype(F32) + gate * projection).astype(BF16)


def solution(mesh):
    try:
        n_x = len({d.coords[0] for d in mesh.devices[:, 0]})
    except AttributeError:
        n_x = 1
    n_sp, n_tp = mesh.shape["sp"], mesh.shape["tp"]
    if n_x < 2 or n_sp % n_x or (n_sp // n_x) % 2:
        n_x = 1
    in_specs = (
        P(("sp", "tp"), None), P("sp", None), P("sp"), P("sp"),
        P("sp", "tp"), P("sp", "tp"), P("sp", "tp"), P(),
        P(None, "tp"), P(None, "tp"), P(None, "tp"), P(), P(), P("tp"), P("tp", None),
    )
    body = functools.partial(shards, n_sp, n_tp, n_x)
    return jax.shard_map(body, mesh=mesh, in_specs=in_specs, out_specs=P(("sp", "tp"), None), check_vma=False)
```

```python
import functools

import jax
import jax.numpy as jnp
from jax import lax
from jax.experimental import pallas as pl
from jax.experimental.pallas import tpu as pltpu
from jax.sharding import PartitionSpec as P

HEAD = 64
GRID = 64
EPSILON = 1e-06
ROTARY_BASE = 10000.0
F32 = jnp.float32
BF16 = jnp.bfloat16
VMEM = pltpu.VMEM


def dot(a, b):
    return jnp.dot(a, b, preferred_element_type=F32)


def remote(src, dst, send, recv, sp, tp):
    return pltpu.make_async_remote_copy(
        src_ref=src,
        dst_ref=dst,
        send_sem=send,
        recv_sem=recv,
        device_id=(sp, tp),
        device_id_type=pl.DeviceIdType.MESH,
    )


def project_kernel(
    n_sp, n_tp, q_heads, k_heads,
    latent_h, context_h, cond, ctx_cond, shift_h, scale_h, gate_h, gain,
    wq_h, wk_h, wv_h, q_gain, k_gain, cos_t, sin_t,
    qz, kv, call, gate_out,
    latent, context, shift_w, scale_w, gate_w, wq, wk, wv,
    lat, ckv, part, total, recv1, recv2, mods,
    s1, r1, s2, r2, sy, ry, sp_own, sp_fwd, rp, sc, rc, loads,
):
    fetch = [
        pltpu.make_async_copy(src, dst, loads.at[i])
        for i, (src, dst) in enumerate(
            (
                (latent_h, latent), (shift_h, shift_w), (scale_h, scale_w), (gate_h, gate_w),
                (context_h, context), (wk_h, wk), (wv_h, wv), (wq_h, wq),
            )
        )
    ]
    for copy in fetch:
        copy.start()
    me = lax.axis_index("sp")
    t = lax.axis_index("tp")
    n_y = n_tp // 2
    y, c = t // 2, t % 2
    partner = y * 2 + 1 - c
    barrier = pltpu.get_barrier_semaphore()

    def greet_sp(j, _):
        pl.semaphore_signal(barrier, inc=1, device_id=(lax.rem(me + j, n_sp), t), device_id_type=pl.DeviceIdType.MESH)
        return 0

    def greet_tp(j, _):
        pl.semaphore_signal(barrier, inc=1, device_id=(me, lax.rem(t + j, n_tp)), device_id_type=pl.DeviceIdType.MESH)
        return 0

    lax.fori_loop(1, n_sp, greet_sp, 0)
    lax.fori_loop(1, n_tp, greet_tp, 0)
    pl.semaphore_wait(barrier, n_sp + n_tp - 2)
    fetch[0].wait()

    def y_copy(k):
        other = lax.rem(y + k, n_y)
        return remote(latent, lat.at[t], sy.at[k], ry.at[t], me, other * 2 + c)

    def y_start(k, _):
        y_copy(k).start()
        return 0

    lax.fori_loop(1, n_y, y_start, 0)
    own_partner = remote(latent, lat.at[t], sp_own, rp.at[t], me, partner)
    own_partner.start()

    rows = lax.broadcasted_iota(jnp.int32, (8, cond.shape[1]), 0)
    a = jnp.broadcast_to(cond[...] / (1.0 + jnp.exp(-cond[...])), rows.shape)
    b = jnp.broadcast_to(ctx_cond[...] / (1.0 + jnp.exp(-ctx_cond[...])), rows.shape)
    first = jnp.where(rows == 0, a, jnp.where(rows == 1, b, 0.0)).astype(BF16)
    second = jnp.where(rows == 2, a, jnp.where(rows == 3, b, 0.0)).astype(BF16)
    third = jnp.where(rows == 4, a, 0.0).astype(BF16)
    for copy in fetch[1:4]:
        copy.wait()
    mine = dot(first, shift_w[...]) + dot(second, scale_w[...]) + dot(third, gate_w[...])
    part[...] = mine
    recv1[me] = mine

    def mod_copy(j):
        return remote(part, recv1.at[me], s1.at[j], r1.at[me], lax.rem(me + j, n_sp), t)

    def mod_start(j, _):
        mod_copy(j).start()
        return 0

    def mod_wait(j, _):
        src = lax.rem(me + j, n_sp)
        pltpu.make_async_copy(recv1.at[src], recv1.at[src], r1.at[src]).wait()
        return 0

    lax.fori_loop(1, n_sp, mod_start, 0)
    lax.fori_loop(1, n_sp, mod_wait, 0)
    summed = lax.fori_loop(1, n_sp, lambda j, s: s + recv1[j], recv1[0])
    total[...] = summed
    recv2[t] = summed

    def tot_copy(j):
        return remote(total, recv2.at[t], s2.at[j], r2.at[t], me, lax.rem(t + j, n_tp))

    def tot_start(j, _):
        tot_copy(j).start()
        return 0

    def tot_wait(j, _):
        src = lax.rem(t + j, n_tp)
        pltpu.make_async_copy(recv2.at[src], recv2.at[src], r2.at[src]).wait()
        return 0

    lax.fori_loop(1, n_tp, tot_start, 0)
    lax.fori_loop(1, n_tp, tot_wait, 0)
    width = total.shape[1]
    for j in range(n_tp):
        mods[:, j * width : (j + 1) * width] = recv2[j]
    gate_out[...] = mods[4:5, :]

    def hidden_of(x, shift_row, scale_row):
        x = x.astype(F32)
        inv = lax.rsqrt(jnp.mean(x * x, axis=-1, keepdims=True) + EPSILON)
        return (
            x * inv * gain[...] * (1.0 + mods[scale_row : scale_row + 1, :])
            + mods[shift_row : shift_row + 1, :]
        ).astype(BF16)

    def head_norm(v, gains):
        w = v.shape[1]
        heads_r = lax.broadcasted_iota(jnp.int32, (w, w), 0) // HEAD
        heads_c = lax.broadcasted_iota(jnp.int32, (w, w), 1) // HEAD
        ones = jnp.where(heads_r == heads_c, 1.0, 0.0).astype(BF16)
        sq = v * v
        hi = sq.astype(BF16)
        rest = sq - hi.astype(F32)
        mid = rest.astype(BF16)
        low = (rest - mid.astype(F32)).astype(BF16)
        mean = (dot(hi, ones) + (dot(mid, ones) + dot(low, ones))) * (1.0 / HEAD)
        return v * lax.rsqrt(mean + EPSILON) * jnp.concatenate([gains] * (w // 128), axis=1)

    def turn(v, cos_v, sin_v):
        w = v.shape[1]
        even = lax.broadcasted_iota(jnp.int32, v.shape, 1) % 2 == 0
        swapped = jnp.where(even, pltpu.roll(v, w - 1, 1), pltpu.roll(v, 1, 1))
        many = w // 128
        return v * jnp.concatenate([cos_v] * many, axis=1) + swapped * jnp.concatenate([sin_v] * many, axis=1)

    k_width = wk.shape[1]
    group = q_heads // k_heads

    def process(tiles, x):
        h = hidden_of(x, 0, 2)
        cos_v = jnp.concatenate([cos_t[tile] for tile in tiles], axis=0)
        sin_v = jnp.concatenate([sin_t[tile] for tile in tiles], axis=0)
        q = turn(head_norm(dot(h, wq[...]), q_gain[...]), cos_v, sin_v)
        per = q.shape[0] // len(tiles)
        low_half = lax.broadcasted_iota(jnp.int32, (q.shape[0], 128), 1) < HEAD
        for head in range(q_heads):
            piece = q[:, (head // 2) * 128 : (head // 2) * 128 + 128].astype(BF16).astype(F32) * HEAD ** (-0.5)
            side = (head // group) % 2
            if head % 2 != side:
                piece = pltpu.roll(piece, HEAD, 1)
            keep = low_half if side == 0 else jnp.logical_not(low_half)
            piece = jnp.where(keep, piece, 0.0)
            for i, tile in enumerate(tiles):
                qz[head, tile] = piece[i * per : (i + 1) * per].astype(BF16)
        k = turn(head_norm(dot(h, wk[...]), k_gain[...]), cos_v, sin_v)
        v = dot(h, wv[...])
        for i, tile in enumerate(tiles):
            kv[tile, :, :k_width] = k[i * per : (i + 1) * per].astype(BF16)
            kv[tile, :, k_width:] = v[i * per : (i + 1) * per].astype(BF16)

    for copy in fetch[4:]:
        copy.wait()
    hc = hidden_of(context[...], 1, 3)
    ckv[:, :k_width] = head_norm(dot(hc, wk[...]), k_gain[...]).astype(BF16)
    ckv[:, k_width:] = dot(hc, wv[...]).astype(BF16)

    def c_copy(j):
        return remote(ckv, call.at[me], sc.at[j], rc.at[me], lax.rem(me + j, n_sp), t)

    def c_start(j, _):
        c_copy(j).start()
        return 0

    lax.fori_loop(1, n_sp, c_start, 0)
    call[me] = ckv[...]

    def pair_of(first, second):
        return jnp.concatenate([first.astype(F32), second.astype(F32)], axis=0)

    pltpu.make_async_copy(lat.at[partner], lat.at[partner], rp.at[partner]).wait()
    process((t, partner), pair_of(latent[...], lat[partner]))

    def others(k, _):
        other = lax.rem(y + n_y - k, n_y)
        near, far = other * 2 + c, other * 2 + 1 - c
        pltpu.make_async_copy(lat.at[near], lat.at[near], ry.at[near]).wait()
        remote(lat.at[near], lat.at[near], sp_fwd.at[k], rp.at[near], me, partner).start()
        pltpu.make_async_copy(lat.at[far], lat.at[far], rp.at[far]).wait()
        process((near, far), pair_of(lat[near], lat[far]))
        return 0

    lax.fori_loop(1, n_y, others, 0)

    def c_wait(j, _):
        src = lax.rem(me + j, n_sp)
        pltpu.make_async_copy(call.at[src], call.at[src], rc.at[src]).wait()
        c_copy(j).wait_send()
        return 0

    lax.fori_loop(1, n_sp, c_wait, 0)

    def drain_y(k, _):
        y_copy(k).wait_send()
        other = lax.rem(y + n_y - k, n_y)
        near = other * 2 + c
        remote(lat.at[near], lat.at[near], sp_fwd.at[k], rp.at[near], me, partner).wait_send()
        return 0

    lax.fori_loop(1, n_y, drain_y, 0)
    own_partner.wait_send()

    def drain_1(j, _):
        mod_copy(j).wait_send()
        return 0

    def drain_2(j, _):
        tot_copy(j).wait_send()
        return 0

    lax.fori_loop(1, n_sp, drain_1, 0)
    lax.fori_loop(1, n_tp, drain_2, 0)


def ring_position(index, n_z, n_x):
    z, x = index // n_x, index % n_x
    back = n_z * (n_x - 1) + n_z - 1 - z
    out = z * (n_x - 1) + jnp.where(z % 2 == 0, x - 1, n_x - 1 - x)
    return jnp.where(x == 0, back, out)


def ring_index(place, n_z, n_x):
    r, k = place // (n_x - 1), place % (n_x - 1)
    out = r * n_x + jnp.where(r % 2 == 0, 1 + k, n_x - 1 - k)
    back = (n_z - 1 - (place - n_z * (n_x - 1))) * n_x
    return jnp.where(place >= n_z * (n_x - 1), back, out)


def attend_kernel(
    n_sp, n_tp, n_x, q_heads, k_heads, chunks,
    qz, kv, call, lift, wo,
    by_rows, wo_all,
    right, left, m_ref, acc, att,
    s_kv, r_kv, s_wy, r_wy, s_wp, r_wp, s_a, r_a, loc,
):
    me = lax.axis_index("sp")
    t = lax.axis_index("tp")
    n_y = n_tp // 2
    y, c = t // 2, t % 2
    partner = y * 2 + 1 - c
    half = n_sp // 2
    if n_x > 1:
        n_z = n_sp // n_x
        place = ring_position(me, n_z, n_x)
        nxt = ring_index(lax.rem(place + 1, n_sp), n_z, n_x)
        prv = ring_index(lax.rem(place + n_sp - 1, n_sp), n_z, n_x)
    else:
        nxt, prv = lax.rem(me + 1, n_sp), lax.rem(me + n_sp - 1, n_sp)
    barrier = pltpu.get_barrier_semaphore()
    for peer in (nxt, prv):
        pl.semaphore_signal(barrier, inc=1, device_id=(peer, t), device_id_type=pl.DeviceIdType.MESH)

    def greet(j, _):
        pl.semaphore_signal(barrier, inc=1, device_id=(me, lax.rem(t + j, n_tp)), device_id_type=pl.DeviceIdType.MESH)
        return 0

    lax.fori_loop(1, n_tp, greet, 0)
    pl.semaphore_wait(barrier, 2 + n_tp - 1)

    length = kv.shape[0]
    mid = length // 2

    def hop(src, dst, direction, i):
        return remote(src, dst, s_kv.at[direction, i], r_kv.at[direction, i], nxt if direction == 0 else prv, t)

    def sends(i, source_r, source_l):
        return (hop(source_r, right.at[i], 0, i), hop(source_l, left.at[i], 1, i))

    def last_sends(source_r, source_l):
        return (
            hop(source_r.at[pl.ds(0, mid)], right.at[half, pl.ds(0, mid)], 0, half),
            hop(source_l.at[pl.ds(mid, mid)], right.at[half, pl.ds(mid, mid)], 1, half),
        )

    opening = sends(1, kv, kv)
    for copy in opening:
        copy.start()
    own_w = pltpu.make_async_copy(wo, wo_all.at[t], loc.at[0])
    own_w.start()

    def w_y(k, ch):
        other = lax.rem(y + k, n_y)
        return remote(wo.at[ch], wo_all.at[t, ch], s_wy.at[k, ch], r_wy.at[t, ch], me, other * 2 + c)

    def w_own(ch):
        return remote(wo.at[ch], wo_all.at[t, ch], s_wp.at[0, ch], r_wp.at[t, ch], me, partner)

    def w_fwd(k, ch):
        other = lax.rem(y + n_y - k, n_y)
        near = other * 2 + c
        return remote(wo_all.at[near, ch], wo_all.at[near, ch], s_wp.at[k, ch], r_wp.at[near, ch], me, partner)

    for ch in range(chunks):
        for k in range(1, n_y):
            w_y(k, ch).start()
    for ch in range(chunks):
        w_own(ch).start()

    def forward_weight(ch):
        for k in range(1, n_y):
            other = lax.rem(y + n_y - k, n_y)
            near = other * 2 + c
            pltpu.make_async_copy(wo_all.at[near, ch], wo_all.at[near, ch], r_wy.at[near, ch]).wait()
            w_fwd(k, ch).start()

    k_width = kv.shape[1] // 2
    group = q_heads // k_heads
    tile = min(256, length)
    tiles = length // tile

    def attend(blocks, start, lifted):
        def one(head, _):
            lane = pl.multiple_of(head // (2 * group) * 128, 128)
            extra = lift[head]
            spans = [pl.ds(i * tile, tile) for i in range(tiles)]
            olds = [] if start else [m_ref[head, span, :] for span in spans]
            keys = [block[:, pl.ds(lane, 128)] for block in blocks]
            values = [block[:, pl.ds(pl.multiple_of(k_width + lane, 128), 128)] for block in blocks]
            values = [jnp.concatenate([v, jnp.ones_like(v)], axis=1) for v in values]
            scores = [
                [
                    lax.dot_general(
                        qz[head, span, :], k, (((1,), (1,)), ((), ())), preferred_element_type=F32
                    )
                    for k in keys
                ]
                for span in spans
            ]
            tops, outs = [], []
            for i in range(tiles):
                peaks = [jnp.max(s, axis=-1, keepdims=True) for s in scores[i]]
                if lifted:
                    peaks[-1] = peaks[-1] + extra
                top = functools.reduce(jnp.maximum, peaks)
                if not start:
                    top = jnp.maximum(olds[i][:, 0:1], top)
                out = None
                for pos, s in enumerate(scores[i]):
                    base = top - extra if lifted and pos == len(blocks) - 1 else top
                    term = dot(jnp.exp(s - base).astype(BF16), values[pos])
                    out = term if out is None else out + term
                wide = jnp.broadcast_to(top, (tile, 128))
                if not start:
                    f = jnp.exp(olds[i] - wide)
                    out = acc[head, spans[i], :] * jnp.concatenate([f, f], axis=1) + out
                tops.append(wide)
                outs.append(out)
            for i in range(tiles):
                m_ref[head, spans[i], :] = tops[i]
                acc[head, spans[i], :] = outs[i]
            return 0

        lax.fori_loop(0, q_heads, one, 0)

    attend([kv], True, False)

    def wait_pair(i):
        for copy in sends(i, kv, kv):
            copy.wait_recv()

    def step(i, _):
        wait_pair(i)
        for copy in sends(i + 1, right.at[i], left.at[i]):
            copy.start()
        attend([right.at[i], left.at[i]], False, False)
        forward_weight(i - 1)
        return 0

    lax.fori_loop(1, half - 1, step, 0)
    wait_pair(half - 1)
    closing = last_sends(right.at[half - 1], left.at[half - 1])
    for copy in closing:
        copy.start()
    attend([right.at[half - 1], left.at[half - 1]], False, False)
    for ch in range(half - 2, chunks):
        forward_weight(ch)
    for copy in closing:
        copy.wait_recv()
    attend([right.at[half], call], False, True)

    low_half = lax.broadcasted_iota(jnp.int32, (length, 128), 1) < HEAD
    per = length // n_tp

    def normal(head):
        return acc[head, :, :128] / acc[head, :, 128:]

    for two in range(q_heads // 2):
        parts = []
        for head in (2 * two, 2 * two + 1):
            o = normal(head)
            if (head // group) % 2 != head % 2:
                o = pltpu.roll(o, HEAD, 1)
            parts.append(o)
        both = jnp.where(low_half, parts[0], parts[1]).astype(BF16)
        for j in range(n_tp):
            att[j, :, two * 128 : two * 128 + 128] = both[j * per : (j + 1) * per, :]

    def a_copy(j):
        to = lax.rem(t + j, n_tp)
        return remote(att.at[to], by_rows.at[t], s_a.at[j], r_a.at[t], me, to)

    for j in range(1, n_tp):
        a_copy(j).start()
    own_a = pltpu.make_async_copy(att.at[t], by_rows.at[t], loc.at[1])
    own_a.start()
    own_a.wait()
    for j in range(1, n_tp):
        src = lax.rem(t + j, n_tp)
        pltpu.make_async_copy(by_rows.at[src], by_rows.at[src], r_a.at[src]).wait()
    own_w.wait()
    for ch in range(chunks):
        for k in range(n_y):
            far = lax.rem(y + n_y - k, n_y) * 2 + 1 - c
            pltpu.make_async_copy(wo_all.at[far, ch], wo_all.at[far, ch], r_wp.at[far, ch]).wait()
        for k in range(1, n_y):
            w_y(k, ch).wait_send()
            w_fwd(k, ch).wait_send()
        w_own(ch).wait_send()
    for j in range(1, n_tp):
        a_copy(j).wait_send()

    def drain(i, _):
        for copy in sends(i, kv, kv):
            copy.wait_send()
        return 0

    lax.fori_loop(1, half, drain, 0)
    for copy in closing:
        copy.wait_send()


def rotary_tables(offset, count):
    position = offset + jnp.arange(count, dtype=jnp.int32)
    grid_row = (position // GRID).astype(F32)
    grid_column = (position % GRID).astype(F32)
    quarter = HEAD // 4
    frequency = ROTARY_BASE ** (-jnp.arange(quarter, dtype=F32) / quarter)
    angles = jnp.concatenate([grid_row[:, None] * frequency, grid_column[:, None] * frequency], axis=1)
    sign = jnp.where(jnp.arange(HEAD) % 2 == 0, -1.0, 1.0)
    cos_t, sin_t = jnp.repeat(jnp.cos(angles), 2, axis=1), jnp.repeat(jnp.sin(angles), 2, axis=1) * sign
    return jnp.tile(cos_t, (1, 2)), jnp.tile(sin_t, (1, 2))


def shards(
    n_sp, n_tp, n_x,
    latent, context, conditioning, context_conditioning, shift_weight, scale_weight, gate_weight,
    norm_gain, query_weight, key_weight, value_weight, query_gain, key_gain, context_lift, output_weight,
):
    k_heads = key_weight.shape[1] // HEAD
    q_heads = query_weight.shape[1] // HEAD
    if k_heads % 2:
        key_weight = jnp.pad(key_weight, ((0, 0), (0, HEAD)))
        value_weight = jnp.pad(value_weight, ((0, 0), (0, HEAD)))
    rows, model = latent.shape
    length = rows * n_tp
    k_width = key_weight.shape[1]
    c_rows = context.shape[0]
    part_width = shift_weight.shape[1]
    cos_t, sin_t = rotary_tables(lax.axis_index("sp") * length, length)
    vmem = pl.BlockSpec(memory_space=VMEM)
    dma = pltpu.SemaphoreType.DMA
    hbm = pl.BlockSpec(memory_space=pltpu.HBM)
    qz, kv, call, gate = pl.pallas_call(
        functools.partial(project_kernel, n_sp, n_tp, q_heads, k_heads),
        name="project",
        out_shape=(
            jax.ShapeDtypeStruct((q_heads, n_tp, rows, 128), BF16),
            jax.ShapeDtypeStruct((n_tp, rows, 2 * k_width), BF16),
            jax.ShapeDtypeStruct((n_sp, c_rows, 2 * k_width), BF16),
            jax.ShapeDtypeStruct((1, model), F32),
        ),
        in_specs=[hbm, hbm, vmem, vmem, hbm, hbm, hbm, vmem, hbm, hbm, hbm, vmem, vmem, vmem, vmem],
        out_specs=(vmem,) * 4,
        scratch_shapes=[
            VMEM(latent.shape, BF16), VMEM(context.shape, BF16),
            VMEM(shift_weight.shape, BF16), VMEM(scale_weight.shape, BF16), VMEM(gate_weight.shape, BF16),
            VMEM(query_weight.shape, BF16), VMEM(key_weight.shape, BF16), VMEM(value_weight.shape, BF16),
            VMEM((n_tp, rows, model), BF16),
            VMEM((c_rows, 2 * k_width), BF16),
            VMEM((8, part_width), F32),
            VMEM((8, part_width), F32),
            VMEM((n_sp, 8, part_width), F32),
            VMEM((n_tp, 8, part_width), F32),
            VMEM((8, model), F32),
            dma((n_sp,)), dma((n_sp,)), dma((n_tp,)), dma((n_tp,)),
            dma((n_tp,)), dma((n_tp,)), dma, dma((n_tp,)), dma((n_tp,)),
            dma((n_sp,)), dma((n_sp,)), dma((8,)),
        ],
        compiler_params=pltpu.CompilerParams(
            collective_id=0, has_side_effects=True, vmem_limit_bytes=48 * 1024 * 1024
        ),
    )(
        latent, context, conditioning[None], context_conditioning[None],
        shift_weight, scale_weight, gate_weight, norm_gain[None],
        query_weight, key_weight, value_weight,
        jnp.tile(query_gain, 2)[None], jnp.tile(key_gain, 2)[None],
        cos_t.reshape(n_tp, rows, 128), sin_t.reshape(n_tp, rows, 128),
    )
    chunks = max(n_sp // 2, 2)
    o_rows = output_weight.shape[0]
    by_rows, wo_all = pl.pallas_call(
        functools.partial(attend_kernel, n_sp, n_tp, n_x, q_heads, k_heads, chunks),
        name="attend",
        out_shape=(
            jax.ShapeDtypeStruct((n_tp, rows, q_heads * HEAD), BF16),
            jax.ShapeDtypeStruct((n_tp, chunks, o_rows // chunks, model), BF16),
        ),
        in_specs=[vmem, vmem, vmem, pl.BlockSpec(memory_space=pltpu.SMEM), vmem],
        out_specs=(vmem, pl.BlockSpec(memory_space=pl.ANY)),
        scratch_shapes=[
            VMEM((n_sp // 2 + 1, length, 2 * k_width), BF16),
            VMEM((n_sp // 2, length, 2 * k_width), BF16),
            VMEM((q_heads, length, 128), F32),
            VMEM((q_heads, length, 256), F32),
            VMEM((n_tp, rows, q_heads * HEAD), BF16),
            dma((2, n_sp)), dma((2, n_sp)),
            dma((n_tp, chunks)), dma((n_tp, chunks)), dma((n_tp, chunks)), dma((n_tp, chunks)),
            dma((n_tp,)), dma((n_tp,)), dma((2,)),
        ],
        compiler_params=pltpu.CompilerParams(
            collective_id=1, has_side_effects=True, vmem_limit_bytes=56 * 1024 * 1024
        ),
    )(
        qz.reshape(q_heads, length, 128), kv.reshape(length, 2 * k_width),
        call.reshape(n_sp * c_rows, 2 * k_width), context_lift,
        output_weight.reshape(chunks, o_rows // chunks, model),
    )
    projection = jnp.dot(
        jnp.transpose(by_rows, (1, 0, 2)).reshape(rows, n_tp * o_rows),
        wo_all.reshape(n_tp * o_rows, model),
        preferred_element_type=F32,
    )
    return (latent.astype(F32) + gate * projection).astype(BF16)


def solution(mesh):
    try:
        n_x = len({d.coords[0] for d in mesh.devices[:, 0]})
    except AttributeError:
        n_x = 1
    n_sp, n_tp = mesh.shape["sp"], mesh.shape["tp"]
    if n_x < 2 or n_sp % n_x or (n_sp // n_x) % 2:
        n_x = 1
    in_specs = (
        P(("sp", "tp"), None), P("sp", None), P("sp"), P("sp"),
        P("sp", "tp"), P("sp", "tp"), P("sp", "tp"), P(),
        P(None, "tp"), P(None, "tp"), P(None, "tp"), P(), P(), P("tp"), P("tp", None),
    )
    body = functools.partial(shards, n_sp, n_tp, n_x)
    return jax.shard_map(body, mesh=mesh, in_specs=in_specs, out_specs=P(("sp", "tp"), None), check_vma=False)
```

```python
import functools

import jax
import jax.numpy as jnp
from jax import lax
from jax.experimental import pallas as pl
from jax.experimental.pallas import tpu as pltpu
from jax.sharding import PartitionSpec as P

HEAD = 64
GRID = 64
EPSILON = 1e-06
ROTARY_BASE = 10000.0
F32 = jnp.float32
BF16 = jnp.bfloat16
VMEM = pltpu.VMEM


def dot(a, b):
    return jnp.dot(a, b, preferred_element_type=F32)


def remote(src, dst, send, recv, sp, tp):
    return pltpu.make_async_remote_copy(
        src_ref=src,
        dst_ref=dst,
        send_sem=send,
        recv_sem=recv,
        device_id=(sp, tp),
        device_id_type=pl.DeviceIdType.MESH,
    )


def project_kernel(
    n_sp, n_tp, q_heads, k_heads,
    latent_h, context_h, cond, ctx_cond, shift_h, scale_h, gate_h, gain,
    wq_h, wk_h, wv_h, q_gain, k_gain, cos_t, sin_t,
    qz, kv, call, gate_out,
    latent, context, shift_w, scale_w, gate_w, wq, wk, wv,
    lat, ckv, part, total, recv1, recv2, mods,
    s1, r1, s2, r2, sy, ry, sp_own, sp_fwd, rp, sc, rc, loads,
):
    fetch = [
        pltpu.make_async_copy(src, dst, loads.at[i])
        for i, (src, dst) in enumerate(
            (
                (latent_h, latent), (shift_h, shift_w), (scale_h, scale_w), (gate_h, gate_w),
                (context_h, context), (wk_h, wk), (wv_h, wv), (wq_h, wq),
            )
        )
    ]
    for copy in fetch:
        copy.start()
    me = lax.axis_index("sp")
    t = lax.axis_index("tp")
    n_y = n_tp // 2
    y, c = t // 2, t % 2
    partner = y * 2 + 1 - c
    barrier = pltpu.get_barrier_semaphore()

    def greet_sp(j, _):
        pl.semaphore_signal(barrier, inc=1, device_id=(lax.rem(me + j, n_sp), t), device_id_type=pl.DeviceIdType.MESH)
        return 0

    def greet_tp(j, _):
        pl.semaphore_signal(barrier, inc=1, device_id=(me, lax.rem(t + j, n_tp)), device_id_type=pl.DeviceIdType.MESH)
        return 0

    lax.fori_loop(1, n_sp, greet_sp, 0)
    lax.fori_loop(1, n_tp, greet_tp, 0)
    pl.semaphore_wait(barrier, n_sp + n_tp - 2)
    fetch[0].wait()

    def y_copy(k):
        other = lax.rem(y + k, n_y)
        return remote(latent, lat.at[t], sy.at[k], ry.at[t], me, other * 2 + c)

    def y_start(k, _):
        y_copy(k).start()
        return 0

    lax.fori_loop(1, n_y, y_start, 0)
    own_partner = remote(latent, lat.at[t], sp_own, rp.at[t], me, partner)
    own_partner.start()

    rows = lax.broadcasted_iota(jnp.int32, (8, cond.shape[1]), 0)
    a = jnp.broadcast_to(cond[...] / (1.0 + jnp.exp(-cond[...])), rows.shape)
    b = jnp.broadcast_to(ctx_cond[...] / (1.0 + jnp.exp(-ctx_cond[...])), rows.shape)
    first = jnp.where(rows == 0, a, jnp.where(rows == 1, b, 0.0)).astype(BF16)
    second = jnp.where(rows == 2, a, jnp.where(rows == 3, b, 0.0)).astype(BF16)
    third = jnp.where(rows == 4, a, 0.0).astype(BF16)
    for copy in fetch[1:4]:
        copy.wait()
    mine = dot(first, shift_w[...]) + dot(second, scale_w[...]) + dot(third, gate_w[...])
    part[...] = mine
    recv1[me] = mine

    def mod_copy(j):
        return remote(part, recv1.at[me], s1.at[j], r1.at[me], lax.rem(me + j, n_sp), t)

    def mod_start(j, _):
        mod_copy(j).start()
        return 0

    def mod_wait(j, _):
        src = lax.rem(me + j, n_sp)
        pltpu.make_async_copy(recv1.at[src], recv1.at[src], r1.at[src]).wait()
        return 0

    lax.fori_loop(1, n_sp, mod_start, 0)
    lax.fori_loop(1, n_sp, mod_wait, 0)
    summed = lax.fori_loop(1, n_sp, lambda j, s: s + recv1[j], recv1[0])
    total[...] = summed
    recv2[t] = summed

    def tot_copy(j):
        return remote(total, recv2.at[t], s2.at[j], r2.at[t], me, lax.rem(t + j, n_tp))

    def tot_start(j, _):
        tot_copy(j).start()
        return 0

    def tot_wait(j, _):
        src = lax.rem(t + j, n_tp)
        pltpu.make_async_copy(recv2.at[src], recv2.at[src], r2.at[src]).wait()
        return 0

    lax.fori_loop(1, n_tp, tot_start, 0)
    lax.fori_loop(1, n_tp, tot_wait, 0)
    width = total.shape[1]
    for j in range(n_tp):
        mods[:, j * width : (j + 1) * width] = recv2[j]
    gate_out[...] = mods[4:5, :]

    def hidden_of(x, shift_row, scale_row):
        x = x.astype(F32)
        inv = lax.rsqrt(jnp.mean(x * x, axis=-1, keepdims=True) + EPSILON)
        return (
            x * inv * gain[...] * (1.0 + mods[scale_row : scale_row + 1, :])
            + mods[shift_row : shift_row + 1, :]
        ).astype(BF16)

    def head_norm(v, gains):
        w = v.shape[1]
        heads_r = lax.broadcasted_iota(jnp.int32, (w, w), 0) // HEAD
        heads_c = lax.broadcasted_iota(jnp.int32, (w, w), 1) // HEAD
        ones = jnp.where(heads_r == heads_c, 1.0, 0.0).astype(BF16)
        sq = v * v
        hi = sq.astype(BF16)
        rest = sq - hi.astype(F32)
        mid = rest.astype(BF16)
        low = (rest - mid.astype(F32)).astype(BF16)
        mean = (dot(hi, ones) + (dot(mid, ones) + dot(low, ones))) * (1.0 / HEAD)
        return v * lax.rsqrt(mean + EPSILON) * jnp.concatenate([gains] * (w // 128), axis=1)

    def turn(v, cos_v, sin_v):
        w = v.shape[1]
        even = lax.broadcasted_iota(jnp.int32, v.shape, 1) % 2 == 0
        swapped = jnp.where(even, pltpu.roll(v, w - 1, 1), pltpu.roll(v, 1, 1))
        many = w // 128
        return v * jnp.concatenate([cos_v] * many, axis=1) + swapped * jnp.concatenate([sin_v] * many, axis=1)

    k_width = wk.shape[1]
    group = q_heads // k_heads

    def process(tiles, x):
        h = hidden_of(x, 0, 2)
        cos_v = jnp.concatenate([cos_t[tile] for tile in tiles], axis=0)
        sin_v = jnp.concatenate([sin_t[tile] for tile in tiles], axis=0)
        q = turn(head_norm(dot(h, wq[...]), q_gain[...]), cos_v, sin_v)
        per = q.shape[0] // len(tiles)
        low_half = lax.broadcasted_iota(jnp.int32, (q.shape[0], 128), 1) < HEAD
        for head in range(q_heads):
            piece = q[:, (head // 2) * 128 : (head // 2) * 128 + 128].astype(BF16).astype(F32) * HEAD ** (-0.5)
            side = (head // group) % 2
            if head % 2 != side:
                piece = pltpu.roll(piece, HEAD, 1)
            keep = low_half if side == 0 else jnp.logical_not(low_half)
            piece = jnp.where(keep, piece, 0.0)
            for i, tile in enumerate(tiles):
                qz[head, tile] = piece[i * per : (i + 1) * per].astype(BF16)
        k = turn(head_norm(dot(h, wk[...]), k_gain[...]), cos_v, sin_v)
        v = dot(h, wv[...])
        for i, tile in enumerate(tiles):
            kv[tile, :, :k_width] = k[i * per : (i + 1) * per].astype(BF16)
            kv[tile, :, k_width:] = v[i * per : (i + 1) * per].astype(BF16)

    for copy in fetch[4:]:
        copy.wait()
    hc = hidden_of(context[...], 1, 3)
    ckv[:, :k_width] = head_norm(dot(hc, wk[...]), k_gain[...]).astype(BF16)
    ckv[:, k_width:] = dot(hc, wv[...]).astype(BF16)

    def c_copy(j):
        return remote(ckv, call.at[me], sc.at[j], rc.at[me], lax.rem(me + j, n_sp), t)

    def c_start(j, _):
        c_copy(j).start()
        return 0

    lax.fori_loop(1, n_sp, c_start, 0)
    call[me] = ckv[...]

    def pair_of(first, second):
        return jnp.concatenate([first.astype(F32), second.astype(F32)], axis=0)

    pltpu.make_async_copy(lat.at[partner], lat.at[partner], rp.at[partner]).wait()
    process((t, partner), pair_of(latent[...], lat[partner]))

    def others(k, _):
        other = lax.rem(y + n_y - k, n_y)
        near, far = other * 2 + c, other * 2 + 1 - c
        pltpu.make_async_copy(lat.at[near], lat.at[near], ry.at[near]).wait()
        remote(lat.at[near], lat.at[near], sp_fwd.at[k], rp.at[near], me, partner).start()
        pltpu.make_async_copy(lat.at[far], lat.at[far], rp.at[far]).wait()
        process((near, far), pair_of(lat[near], lat[far]))
        return 0

    lax.fori_loop(1, n_y, others, 0)

    def c_wait(j, _):
        src = lax.rem(me + j, n_sp)
        pltpu.make_async_copy(call.at[src], call.at[src], rc.at[src]).wait()
        c_copy(j).wait_send()
        return 0

    lax.fori_loop(1, n_sp, c_wait, 0)

    def drain_y(k, _):
        y_copy(k).wait_send()
        other = lax.rem(y + n_y - k, n_y)
        near = other * 2 + c
        remote(lat.at[near], lat.at[near], sp_fwd.at[k], rp.at[near], me, partner).wait_send()
        return 0

    lax.fori_loop(1, n_y, drain_y, 0)
    own_partner.wait_send()

    def drain_1(j, _):
        mod_copy(j).wait_send()
        return 0

    def drain_2(j, _):
        tot_copy(j).wait_send()
        return 0

    lax.fori_loop(1, n_sp, drain_1, 0)
    lax.fori_loop(1, n_tp, drain_2, 0)


def ring_position(index, n_z, n_x):
    z, x = index // n_x, index % n_x
    back = n_z * (n_x - 1) + n_z - 1 - z
    out = z * (n_x - 1) + jnp.where(z % 2 == 0, x - 1, n_x - 1 - x)
    return jnp.where(x == 0, back, out)


def ring_index(place, n_z, n_x):
    r, k = place // (n_x - 1), place % (n_x - 1)
    out = r * n_x + jnp.where(r % 2 == 0, 1 + k, n_x - 1 - k)
    back = (n_z - 1 - (place - n_z * (n_x - 1))) * n_x
    return jnp.where(place >= n_z * (n_x - 1), back, out)


def attend_kernel(
    n_sp, n_tp, n_x, q_heads, k_heads, chunks,
    qz, kv, call, lift, wo,
    by_rows, wo_all,
    right, left, m_ref, acc, att,
    s_kv, r_kv, s_wy, r_wy, s_wp, r_wp, s_a, r_a, loc,
):
    me = lax.axis_index("sp")
    t = lax.axis_index("tp")
    n_y = n_tp // 2
    y, c = t // 2, t % 2
    partner = y * 2 + 1 - c
    half = n_sp // 2
    if n_x > 1:
        n_z = n_sp // n_x
        place = ring_position(me, n_z, n_x)
        nxt = ring_index(lax.rem(place + 1, n_sp), n_z, n_x)
        prv = ring_index(lax.rem(place + n_sp - 1, n_sp), n_z, n_x)
    else:
        nxt, prv = lax.rem(me + 1, n_sp), lax.rem(me + n_sp - 1, n_sp)
    barrier = pltpu.get_barrier_semaphore()
    for peer in (nxt, prv):
        pl.semaphore_signal(barrier, inc=1, device_id=(peer, t), device_id_type=pl.DeviceIdType.MESH)

    def greet(j, _):
        pl.semaphore_signal(barrier, inc=1, device_id=(me, lax.rem(t + j, n_tp)), device_id_type=pl.DeviceIdType.MESH)
        return 0

    lax.fori_loop(1, n_tp, greet, 0)
    pl.semaphore_wait(barrier, 2 + n_tp - 1)

    length = kv.shape[0]
    mid = length // 2

    def hop(src, dst, direction, i):
        return remote(src, dst, s_kv.at[direction, i], r_kv.at[direction, i], nxt if direction == 0 else prv, t)

    def sends(i, source_r, source_l):
        return (hop(source_r, right.at[i], 0, i), hop(source_l, left.at[i], 1, i))

    def last_sends(source_r, source_l):
        return (
            hop(source_r.at[pl.ds(0, mid)], right.at[half, pl.ds(0, mid)], 0, half),
            hop(source_l.at[pl.ds(mid, mid)], right.at[half, pl.ds(mid, mid)], 1, half),
        )

    opening = sends(1, kv, kv)
    for copy in opening:
        copy.start()
    own_w = pltpu.make_async_copy(wo, wo_all.at[t], loc.at[0])
    own_w.start()

    def w_y(k, ch):
        other = lax.rem(y + k, n_y)
        return remote(wo.at[ch], wo_all.at[t, ch], s_wy.at[k, ch], r_wy.at[t, ch], me, other * 2 + c)

    def w_own(ch):
        return remote(wo.at[ch], wo_all.at[t, ch], s_wp.at[0, ch], r_wp.at[t, ch], me, partner)

    def w_fwd(k, ch):
        other = lax.rem(y + n_y - k, n_y)
        near = other * 2 + c
        return remote(wo_all.at[near, ch], wo_all.at[near, ch], s_wp.at[k, ch], r_wp.at[near, ch], me, partner)

    for ch in range(chunks):
        for k in range(1, n_y):
            w_y(k, ch).start()
    for ch in range(chunks):
        w_own(ch).start()

    def forward_weight(ch):
        for k in range(1, n_y):
            other = lax.rem(y + n_y - k, n_y)
            near = other * 2 + c
            pltpu.make_async_copy(wo_all.at[near, ch], wo_all.at[near, ch], r_wy.at[near, ch]).wait()
            w_fwd(k, ch).start()

    k_width = kv.shape[1] // 2
    group = q_heads // k_heads
    tile = min(256, length)
    tiles = length // tile

    def attend(blocks, start, lifted):
        def one(head, _):
            lane = pl.multiple_of(head // (2 * group) * 128, 128)
            extra = lift[head]
            spans = [pl.ds(i * tile, tile) for i in range(tiles)]
            olds = [] if start else [m_ref[head, span, :] for span in spans]
            keys = [block[:, pl.ds(lane, 128)] for block in blocks]
            values = [block[:, pl.ds(pl.multiple_of(k_width + lane, 128), 128)] for block in blocks]
            values = [jnp.concatenate([v, jnp.ones_like(v)], axis=1) for v in values]
            scores = [
                [
                    lax.dot_general(
                        qz[head, span, :], k, (((1,), (1,)), ((), ())), preferred_element_type=F32
                    )
                    for k in keys
                ]
                for span in spans
            ]
            tops, outs = [], []
            for i in range(tiles):
                peaks = [jnp.max(s, axis=-1, keepdims=True) for s in scores[i]]
                if lifted:
                    peaks[-1] = peaks[-1] + extra
                top = functools.reduce(jnp.maximum, peaks)
                if not start:
                    top = jnp.maximum(olds[i][:, 0:1], top)
                out = None
                for pos, s in enumerate(scores[i]):
                    base = top - extra if lifted and pos == len(blocks) - 1 else top
                    term = dot(jnp.exp(s - base).astype(BF16), values[pos])
                    out = term if out is None else out + term
                wide = jnp.broadcast_to(top, (tile, 128))
                if not start:
                    f = jnp.exp(olds[i] - wide)
                    out = acc[head, spans[i], :] * jnp.concatenate([f, f], axis=1) + out
                tops.append(wide)
                outs.append(out)
            for i in range(tiles):
                m_ref[head, spans[i], :] = tops[i]
                acc[head, spans[i], :] = outs[i]
            return 0

        lax.fori_loop(0, q_heads, one, 0)

    attend([kv], True, False)

    def wait_pair(i):
        for copy in sends(i, kv, kv):
            copy.wait_recv()

    def step(i, _):
        wait_pair(i)
        for copy in sends(i + 1, right.at[i], left.at[i]):
            copy.start()
        attend([right.at[i], left.at[i]], False, False)
        forward_weight(i - 1)
        return 0

    lax.fori_loop(1, half - 1, step, 0)
    wait_pair(half - 1)
    closing = last_sends(right.at[half - 1], left.at[half - 1])
    for copy in closing:
        copy.start()
    attend([right.at[half - 1], left.at[half - 1]], False, False)
    for ch in range(half - 2, chunks):
        forward_weight(ch)
    for copy in closing:
        copy.wait_recv()
    attend([right.at[half], call], False, True)

    low_half = lax.broadcasted_iota(jnp.int32, (length, 128), 1) < HEAD
    per = length // n_tp

    def normal(head):
        return acc[head, :, :128] / acc[head, :, 128:]

    for two in range(q_heads // 2):
        parts = []
        for head in (2 * two, 2 * two + 1):
            o = normal(head)
            if (head // group) % 2 != head % 2:
                o = pltpu.roll(o, HEAD, 1)
            parts.append(o)
        both = jnp.where(low_half, parts[0], parts[1]).astype(BF16)
        for j in range(n_tp):
            att[j, :, two * 128 : two * 128 + 128] = both[j * per : (j + 1) * per, :]

    def a_copy(j):
        to = lax.rem(t + j, n_tp)
        return remote(att.at[to], by_rows.at[t], s_a.at[j], r_a.at[t], me, to)

    for j in range(1, n_tp):
        a_copy(j).start()
    own_a = pltpu.make_async_copy(att.at[t], by_rows.at[t], loc.at[1])
    own_a.start()
    own_a.wait()
    for j in range(1, n_tp):
        src = lax.rem(t + j, n_tp)
        pltpu.make_async_copy(by_rows.at[src], by_rows.at[src], r_a.at[src]).wait()
    own_w.wait()
    for ch in range(chunks):
        for k in range(n_y):
            far = lax.rem(y + n_y - k, n_y) * 2 + 1 - c
            pltpu.make_async_copy(wo_all.at[far, ch], wo_all.at[far, ch], r_wp.at[far, ch]).wait()
        for k in range(1, n_y):
            w_y(k, ch).wait_send()
            w_fwd(k, ch).wait_send()
        w_own(ch).wait_send()
    for j in range(1, n_tp):
        a_copy(j).wait_send()

    def drain(i, _):
        for copy in sends(i, kv, kv):
            copy.wait_send()
        return 0

    lax.fori_loop(1, half, drain, 0)
    for copy in closing:
        copy.wait_send()


def rotary_tables(offset, count):
    position = offset + jnp.arange(count, dtype=jnp.int32)
    grid_row = (position // GRID).astype(F32)
    grid_column = (position % GRID).astype(F32)
    quarter = HEAD // 4
    frequency = ROTARY_BASE ** (-jnp.arange(quarter, dtype=F32) / quarter)
    angles = jnp.concatenate([grid_row[:, None] * frequency, grid_column[:, None] * frequency], axis=1)
    sign = jnp.where(jnp.arange(HEAD) % 2 == 0, -1.0, 1.0)
    cos_t, sin_t = jnp.repeat(jnp.cos(angles), 2, axis=1), jnp.repeat(jnp.sin(angles), 2, axis=1) * sign
    return jnp.tile(cos_t, (1, 2)), jnp.tile(sin_t, (1, 2))


def shards(
    n_sp, n_tp, n_x,
    latent, context, conditioning, context_conditioning, shift_weight, scale_weight, gate_weight,
    norm_gain, query_weight, key_weight, value_weight, query_gain, key_gain, context_lift, output_weight,
):
    k_heads = key_weight.shape[1] // HEAD
    q_heads = query_weight.shape[1] // HEAD
    if k_heads % 2:
        key_weight = jnp.pad(key_weight, ((0, 0), (0, HEAD)))
        value_weight = jnp.pad(value_weight, ((0, 0), (0, HEAD)))
    rows, model = latent.shape
    length = rows * n_tp
    k_width = key_weight.shape[1]
    c_rows = context.shape[0]
    part_width = shift_weight.shape[1]
    cos_t, sin_t = rotary_tables(lax.axis_index("sp") * length, length)
    vmem = pl.BlockSpec(memory_space=VMEM)
    dma = pltpu.SemaphoreType.DMA
    hbm = pl.BlockSpec(memory_space=pltpu.HBM)
    qz, kv, call, gate = pl.pallas_call(
        functools.partial(project_kernel, n_sp, n_tp, q_heads, k_heads),
        name="project",
        out_shape=(
            jax.ShapeDtypeStruct((q_heads, n_tp, rows, 128), BF16),
            jax.ShapeDtypeStruct((n_tp, rows, 2 * k_width), BF16),
            jax.ShapeDtypeStruct((n_sp, c_rows, 2 * k_width), BF16),
            jax.ShapeDtypeStruct((1, model), F32),
        ),
        in_specs=[hbm, hbm, vmem, vmem, hbm, hbm, hbm, vmem, hbm, hbm, hbm, vmem, vmem, vmem, vmem],
        out_specs=(vmem,) * 4,
        scratch_shapes=[
            VMEM(latent.shape, BF16), VMEM(context.shape, BF16),
            VMEM(shift_weight.shape, BF16), VMEM(scale_weight.shape, BF16), VMEM(gate_weight.shape, BF16),
            VMEM(query_weight.shape, BF16), VMEM(key_weight.shape, BF16), VMEM(value_weight.shape, BF16),
            VMEM((n_tp, rows, model), BF16),
            VMEM((c_rows, 2 * k_width), BF16),
            VMEM((8, part_width), F32),
            VMEM((8, part_width), F32),
            VMEM((n_sp, 8, part_width), F32),
            VMEM((n_tp, 8, part_width), F32),
            VMEM((8, model), F32),
            dma((n_sp,)), dma((n_sp,)), dma((n_tp,)), dma((n_tp,)),
            dma((n_tp,)), dma((n_tp,)), dma, dma((n_tp,)), dma((n_tp,)),
            dma((n_sp,)), dma((n_sp,)), dma((8,)),
        ],
        compiler_params=pltpu.CompilerParams(
            collective_id=0, has_side_effects=True, vmem_limit_bytes=67043328
        ),
    )(
        latent, context, conditioning[None], context_conditioning[None],
        shift_weight, scale_weight, gate_weight, norm_gain[None],
        query_weight, key_weight, value_weight,
        jnp.tile(query_gain, 2)[None], jnp.tile(key_gain, 2)[None],
        cos_t.reshape(n_tp, rows, 128), sin_t.reshape(n_tp, rows, 128),
    )
    chunks = max(n_sp // 2, 2)
    o_rows = output_weight.shape[0]
    by_rows, wo_all = pl.pallas_call(
        functools.partial(attend_kernel, n_sp, n_tp, n_x, q_heads, k_heads, chunks),
        name="attend",
        out_shape=(
            jax.ShapeDtypeStruct((n_tp, rows, q_heads * HEAD), BF16),
            jax.ShapeDtypeStruct((n_tp, chunks, o_rows // chunks, model), BF16),
        ),
        in_specs=[vmem, vmem, vmem, pl.BlockSpec(memory_space=pltpu.SMEM), vmem],
        out_specs=(vmem, pl.BlockSpec(memory_space=pl.ANY)),
        scratch_shapes=[
            VMEM((n_sp // 2 + 1, length, 2 * k_width), BF16),
            VMEM((n_sp // 2, length, 2 * k_width), BF16),
            VMEM((q_heads, length, 128), F32),
            VMEM((q_heads, length, 256), F32),
            VMEM((n_tp, rows, q_heads * HEAD), BF16),
            dma((2, n_sp)), dma((2, n_sp)),
            dma((n_tp, chunks)), dma((n_tp, chunks)), dma((n_tp, chunks)), dma((n_tp, chunks)),
            dma((n_tp,)), dma((n_tp,)), dma((2,)),
        ],
        compiler_params=pltpu.CompilerParams(
            collective_id=1, has_side_effects=True, vmem_limit_bytes=56 * 1024 * 1024
        ),
    )(
        qz.reshape(q_heads, length, 128), kv.reshape(length, 2 * k_width),
        call.reshape(n_sp * c_rows, 2 * k_width), context_lift,
        output_weight.reshape(chunks, o_rows // chunks, model),
    )
    projection = jnp.dot(
        jnp.transpose(by_rows, (1, 0, 2)).reshape(rows, n_tp * o_rows),
        wo_all.reshape(n_tp * o_rows, model),
        preferred_element_type=F32,
    )
    return (latent.astype(F32) + gate * projection).astype(BF16)


def solution(mesh):
    try:
        n_x = len({d.coords[0] for d in mesh.devices[:, 0]})
    except AttributeError:
        n_x = 1
    n_sp, n_tp = mesh.shape["sp"], mesh.shape["tp"]
    if n_x < 2 or n_sp % n_x or (n_sp // n_x) % 2:
        n_x = 1
    in_specs = (
        P(("sp", "tp"), None), P("sp", None), P("sp"), P("sp"),
        P("sp", "tp"), P("sp", "tp"), P("sp", "tp"), P(),
        P(None, "tp"), P(None, "tp"), P(None, "tp"), P(), P(), P("tp"), P("tp", None),
    )
    body = functools.partial(shards, n_sp, n_tp, n_x)
    return jax.shard_map(body, mesh=mesh, in_specs=in_specs, out_specs=P(("sp", "tp"), None), check_vma=False)
```
